32 devices in a mesh: sp: 8 (over z, y), tp: 4 (over x, core).
Axes of the slice: x: 2, y: 2, z: 4, core: 2. Of those that a mesh axis runs over, the one named last changes fastest.
Arguments:
- tokens: bfloat16 [4096, 2048], P('sp'), may hold values from -6 to 6
- input_norm_gain: bfloat16 [2048], replicated, may hold values from 0.099609375 to 1.8984375
- gate_matrix: bfloat16 [2048, 1024], P('sp', 'tp'), may hold values from -0.125 to 0.125
- input_matrix: bfloat16 [2048, 1024], P('sp', 'tp'), may hold values from -0.125 to 0.125
- write_matrix: bfloat16 [2048, 512], P('sp', 'tp'), may hold values from -0.125 to 0.125
- read_matrix: bfloat16 [2048, 512], P('sp', 'tp'), may hold values from -0.125 to 0.125
- step_matrix: bfloat16 [2048, 16], P('sp'), may hold values from -0.125 to 0.125
- pooling_input_matrix: bfloat16 [2048, 1024], P('sp', 'tp'), may hold values from -0.125 to 0.125
- input_conv_taps: bfloat16 [3, 1024], P(None, 'tp'), may hold values from -3.5 to 3.5
- write_conv_taps: bfloat16 [3, 512], P(None, 'tp'), may hold values from -3.5 to 3.5
- read_conv_taps: bfloat16 [3, 512], P(None, 'tp'), may hold values from -3.5 to 3.5
- head_step_base: float32 [16], P('tp'), may hold values from 0 to 1, as said below
- position_step_factor: float32 [4096], P('sp'), may hold values from 0 to 3, as said below
- position_log_decay: float32 [4096, 16], P('sp', 'tp'), may hold values from -2 to 0, as said below
- gated_norm_gain: bfloat16 [1024], P('tp'), may hold values from 0.099609375 to 1.8984375
- group_linear_maps: bfloat16 [4, 256, 256], P('tp'), may hold values from -0.375 to 0.375
- pooling_channel_scale: bfloat16 [1024], P('tp'), may hold values from 0.099609375 to 1.8984375
- state_output_matrix: bfloat16 [1024, 2048], P('tp', 'sp'), may hold values from -0.125 to 0.125
- pooling_output_matrix: bfloat16 [1024, 2048], P('tp', 'sp'), may hold values from -0.125 to 0.125
Outputs:
- mixed: bfloat16 [4096, 2048], P(('sp', 'tp'))
The draws below stay inside these ranges and needn't reach their ends.
Inputs may be any that keep to these rules, and one draw needn't show every extreme that they name: `head_step_base`: positive. `position_step_factor`: positive. `position_log_decay`: never positive.
All inputs are finite; a program needn't handle non-finite values.
Results may differ from the reference program's by a relative error of at most 0.012.
Values may be sent and summed in bfloat16 or wider, within the bound.
A program may use at most 64 MiB of HBM per device.

```python
import jax
import jax.numpy as jnp
from jax import lax

D = 2048
SSD_INNER = 1024
HEAD_DIM = 64
GROUPS = 4
STATE = 128
POOL_WIDTH = 1024
POOL_GROUPS = 4
BLOCK = 128
TOK_DEV = 512
SSM_STREAMS = 16
PG = 256
TOKEN_TOTAL = 4096


def draw_tokens(key, part):
    key_noise, key_direction = jax.random.split(key, 2)
    segment = TOK_DEV // 2
    directions = jax.random.normal(key_direction, (TOKEN_TOTAL // segment, D), jnp.float32)
    noise = jax.random.normal(key_noise, (TOKEN_TOTAL, D), jnp.float32)
    offsets = directions
    return jnp.clip(noise + jnp.repeat(offsets, segment, axis=0), -6.0, 6.0).astype(jnp.bfloat16)


def draw_head_step_base(key, part):
    key_slow, key_fast, key_pick = jax.random.split(key, 3)
    slow_rates = jnp.exp(jax.random.uniform(key_slow, (SSM_STREAMS,), jnp.float32, jnp.log(0.1 / TOKEN_TOTAL), jnp.log(1.0 / TOKEN_TOTAL)))
    fast_rates = jnp.exp(jax.random.uniform(key_fast, (SSM_STREAMS,), jnp.float32, jnp.log(0.015), jnp.log(0.04)))
    ranking = jax.random.permutation(key_pick, SSM_STREAMS)
    chosen = ranking < SSM_STREAMS // 2
    return jnp.where(chosen, fast_rates, slow_rates)


def draw_position_step_factor(key, part):
    segment = TOK_DEV // 2
    factors = jnp.exp(jax.random.uniform(key, (TOKEN_TOTAL // segment,), jnp.float32, -0.7, 0.7))
    return jnp.repeat(factors, segment)


def draw_position_log_decay(key, part):
    key_spot, key_depth = jax.random.split(key, 2)
    site_offsets = jax.random.randint(key_spot, (4, SSM_STREAMS), 0, TOKEN_TOTAL)
    stack_levels = jax.random.uniform(key_depth, (4, SSM_STREAMS), jnp.float32, -0.5, -0.22)
    location_indices = jnp.arange(TOKEN_TOTAL)[:, None]
    fading_spans = jnp.zeros((TOKEN_TOTAL, SSM_STREAMS), jnp.float32)
    for entry_number in range(4):
        fading_spans = fading_spans + jnp.where(location_indices == site_offsets[entry_number][None, :], stack_levels[entry_number][None, :], 0.0)
    return fading_spans


def levels(stream_key, shape, cuts, least, top_value):
    def one(axis_at, parts):
        draws = jax.random.uniform(jax.random.fold_in(jax.random.fold_in(stream_key, 6), axis_at), (parts,), jnp.float32, least / len(cuts), top_value / len(cuts))
        return jnp.repeat(jnp.exp(draws), shape[axis_at] // parts).reshape((-1,) + (1,) * (len(shape) - axis_at - 1))

    loudness = one(*cuts[0])
    for cut in cuts[1:]:
        loudness = loudness * one(*cut)
    return loudness


def scatter_about(key, dims, deviation, bound, cuts=(), kind=jnp.bfloat16):
    factor_of = levels(key, dims, cuts, -0.22, 0.18) if cuts else 1.0
    result = jax.random.normal(key, dims, jnp.float32) * deviation * factor_of
    return jnp.minimum(jnp.maximum(result, -bound), bound).astype(kind)


def setup_inputs(seed: int = 0) -> dict:
    seeds = jax.random.split(jax.random.key(seed), 20)
    return {
        "tokens": draw_tokens(jax.random.fold_in(seeds[19], 71), 0),
        "input_norm_gain": jnp.clip(1.0 + 0.18 * jax.random.normal(seeds[1], (D,), jnp.float32), 0.099609375, 1.8984375).astype(jnp.bfloat16),
        "gate_matrix": scatter_about(seeds[2], (D, SSD_INNER), D ** -0.5, 0.125, ((0, 8), (1, 4))),
        "input_matrix": scatter_about(seeds[3], (D, SSD_INNER), D ** -0.5, 0.125, ((0, 8), (1, 4))),
        "write_matrix": scatter_about(seeds[4], (D, GROUPS * STATE), D ** -0.5, 0.125, ((0, 8), (1, 4))),
        "read_matrix": scatter_about(seeds[5], (D, GROUPS * STATE), D ** -0.5, 0.125, ((0, 8), (1, 4))),
        "step_matrix": scatter_about(seeds[6], (D, SSM_STREAMS), D ** -0.5, 0.125, ((0, 8),)),
        "pooling_input_matrix": scatter_about(seeds[7], (D, POOL_WIDTH), D ** -0.5, 0.125, ((0, 8), (1, 4))),
        "input_conv_taps": scatter_about(seeds[8], (3, SSD_INNER), 3 ** -0.5, 3.5, ((1, 4),)),
        "write_conv_taps": scatter_about(seeds[9], (3, GROUPS * STATE), 3 ** -0.5, 3.5, ((1, 4),)),
        "read_conv_taps": scatter_about(seeds[10], (3, GROUPS * STATE), 3 ** -0.5, 3.5, ((1, 4),)),
        "head_step_base": draw_head_step_base(jax.random.fold_in(seeds[19], 71), 0),
        "position_step_factor": draw_position_step_factor(jax.random.fold_in(seeds[19], 71), 0),
        "position_log_decay": draw_position_log_decay(jax.random.fold_in(seeds[19], 71), 0),
        "gated_norm_gain": jnp.clip(1.0 + 0.18 * jax.random.normal(seeds[14], (SSD_INNER,), jnp.float32), 0.099609375, 1.8984375).astype(jnp.bfloat16),
        "group_linear_maps": scatter_about(seeds[15], (POOL_GROUPS, PG, PG), PG ** -0.5, 0.375, ((0, 4),)),
        "pooling_channel_scale": jnp.clip(1.0 + 0.18 * jax.random.normal(seeds[16], (POOL_WIDTH,), jnp.float32), 0.099609375, 1.8984375).astype(jnp.bfloat16),
        "state_output_matrix": scatter_about(seeds[17], (SSD_INNER, D), (SSD_INNER + POOL_WIDTH) ** -0.5, 0.125, ((0, 4), (1, 8))),
        "pooling_output_matrix": scatter_about(seeds[18], (POOL_WIDTH, D), (SSD_INNER + POOL_WIDTH) ** -0.5, 0.125, ((0, 4), (1, 8))),
    }


EPSILON = 1e-06
HIGHEST_PRECISION = lax.Precision.HIGHEST

def block_sweep(readers, writers, values, decay_logarithm):
    length = values.shape[0]
    blocks = length // BLOCK
    lower_mask = jnp.tril(jnp.ones((BLOCK, BLOCK), dtype=bool))[:, :, None, None]

    def as_blocks(array):
        return array.reshape((blocks, BLOCK) + array.shape[1:])

    def one_block(carry_state, inputs):
        read_block, write_block, value_block, decay_block = inputs
        running = jnp.cumsum(decay_block, axis=0)
        scores = jnp.einsum('ign,jgn->ijg', read_block, write_block, precision=HIGHEST_PRECISION)
        spread = jnp.where(lower_mask, running[:, None] - running[None, :], -jnp.inf)
        weights = scores[..., None] * jnp.exp(spread)
        within = jnp.einsum('ijgr,jgrp->igrp', weights, value_block, precision=HIGHEST_PRECISION)
        carried = jnp.einsum('ign,grnp->igrp', read_block, carry_state, precision=HIGHEST_PRECISION)
        carried = carried * jnp.exp(running)[..., None]
        block_total = running[-1]
        fading = jnp.exp(block_total[None] - running)
        inflow = jnp.einsum('jgn,jgrp->grnp', write_block, value_block * fading[..., None], precision=HIGHEST_PRECISION)
        return (carry_state * jnp.exp(block_total)[..., None, None] + inflow, within + carried)
    initial = jnp.zeros((values.shape[1], values.shape[2], writers.shape[2], values.shape[3]), jnp.float32)
    last_state, outputs = lax.scan(one_block, initial, (as_blocks(readers), as_blocks(writers), as_blocks(values), as_blocks(decay_logarithm)))
    return (outputs.reshape(values.shape), last_state)

def centred_conv(signal, taps):
    length = signal.shape[0]
    padded = jnp.pad(signal, ((1, 1), (0, 0)))
    return padded[0:length] * taps[0] + padded[1:length + 1] * taps[1] + padded[2:length + 2] * taps[2]

def reference(tokens, input_norm_gain, gate_matrix, input_matrix, write_matrix, read_matrix, step_matrix, pooling_input_matrix, input_conv_taps, write_conv_taps, read_conv_taps, head_step_base, position_step_factor, position_log_decay, gated_norm_gain, group_linear_maps, pooling_channel_scale, state_output_matrix, pooling_output_matrix):
    f32 = jnp.float32
    bf16 = jnp.bfloat16
    wide = tokens.astype(f32)
    normed = (wide * lax.rsqrt(lax.optimization_barrier(jnp.mean(wide * wide, axis=1, keepdims=True)) + EPSILON) * input_norm_gain.astype(f32)).astype(bf16)

    def project(weight):
        return jnp.dot(normed, weight, preferred_element_type=f32)
    gate_pre = project(gate_matrix).astype(bf16)
    input_pre = project(input_matrix).astype(bf16)
    write_pre = project(write_matrix).astype(bf16)
    read_pre = project(read_matrix).astype(bf16)
    pool_in = project(pooling_input_matrix).astype(bf16)
    step_raw = project(step_matrix)
    inputs = jax.nn.silu(centred_conv(input_pre.astype(f32), input_conv_taps.astype(f32))).astype(bf16)
    writers = jax.nn.silu(centred_conv(write_pre.astype(f32), write_conv_taps.astype(f32))).astype(bf16)
    readers = jax.nn.silu(centred_conv(read_pre.astype(f32), read_conv_taps.astype(f32))).astype(bf16)
    step_size = head_step_base[None, :] * jax.nn.softplus(step_raw) * position_step_factor[:, None]
    decay_logarithm = position_log_decay - step_size
    repeat_count = SSM_STREAMS // GROUPS
    values = (inputs.astype(f32).reshape(TOKEN_TOTAL, SSM_STREAMS, HEAD_DIM) * step_size[..., None]).reshape(TOKEN_TOTAL, GROUPS, repeat_count, HEAD_DIM)
    grouped_decay = decay_logarithm.reshape(TOKEN_TOTAL, GROUPS, repeat_count)
    readers_f = readers.astype(f32).reshape(TOKEN_TOTAL, GROUPS, STATE)
    writers_f = writers.astype(f32).reshape(TOKEN_TOTAL, GROUPS, STATE)
    ahead, unused_a = block_sweep(readers_f, writers_f, values, grouped_decay)
    behind, unused_b = block_sweep(jnp.flip(readers_f, 0), jnp.flip(writers_f, 0), jnp.flip(values, 0), jnp.flip(grouped_decay, 0))
    scanned = (ahead + jnp.flip(behind, 0)).reshape(TOKEN_TOTAL, SSD_INNER)
    gated = scanned * jax.nn.silu(gate_pre.astype(f32))
    state_mixed = (gated * lax.rsqrt(lax.optimization_barrier(jnp.mean(gated * gated, axis=1, keepdims=True)) + EPSILON) * gated_norm_gain.astype(f32)).astype(bf16)
    width_group = POOL_WIDTH // POOL_GROUPS
    reach = 2 ** (POOL_GROUPS - 1)
    grouped_in = pool_in.astype(f32).reshape(TOKEN_TOTAL, POOL_GROUPS, width_group)
    extended = jnp.pad(grouped_in, ((reach, reach), (0, 0), (0, 0)))
    halves = 2 ** jnp.arange(POOL_GROUPS)
    window_sum = jnp.zeros_like(grouped_in)
    for offset in range(-reach, reach):
        taken = ((offset >= -halves) & (offset < halves)).astype(f32)
        window_sum = window_sum + extended[reach + offset:reach + offset + TOKEN_TOTAL] * taken[None, :, None]
    positions = jnp.arange(TOKEN_TOTAL)[:, None]
    counts = (jnp.minimum(positions + halves[None, :], TOKEN_TOTAL) - jnp.maximum(positions - halves[None, :], 0)).astype(f32)
    pooled = (window_sum / counts[..., None] - grouped_in).astype(bf16)
    mapped = jnp.einsum('tgc,gcd->tgd', pooled.astype(f32), group_linear_maps.astype(f32))
    pool_mixed = (mapped.reshape(TOKEN_TOTAL, POOL_WIDTH) * pooling_channel_scale.astype(f32)).astype(bf16)
    summed = jnp.dot(state_mixed, state_output_matrix, preferred_element_type=f32) + jnp.dot(pool_mixed, pooling_output_matrix, preferred_element_type=f32)
    return summed.astype(bf16)
```

```python
import functools

import jax
import jax.numpy as jnp
from jax import lax
from jax.experimental import pallas as pl
from jax.experimental.pallas import tpu as pltpu
from jax.sharding import PartitionSpec as P

HEAD_DIM = 64
SSD_INNER = 1024
EPSILON = 1e-06
HALO = 16
LOGICAL = pl.DeviceIdType.MESH
f32 = jnp.float32
bf16 = jnp.bfloat16
HIGHEST = lax.Precision.HIGHEST


def softplus(v):
    return jnp.maximum(v, 0.0) + jnp.log1p(jnp.exp(-jnp.abs(v)))


def silu(v):
    return v / (1.0 + jnp.exp(-v))


def mixer_kernel(
    n, t_size, dims,
    tok, gain, w, stept, taps, base, psf, pld, ngain, maps, pscale,
    out,
    halo, xn, wbuf, sbuf, acc, s_out, s_in, tot_out, tot_in, ent, lea, xs, xr, qs, qr,
    w_send, w_recv, st_send, st_recv, h_send, h_recv, s_send, s_recv, t_send, t_recv,
    x_send, x_recv, q_send, q_recv,
):
    rows, inner, state, pool = dims
    me = lax.axis_index("sp")
    tp = lax.axis_index("tp")
    high = n // 2
    h, l = me // 2, me % 2
    depth = w.shape[0]
    width = tok.shape[1]

    barrier = pltpu.get_barrier_semaphore()

    def greet(k, c):
        pl.semaphore_signal(barrier, inc=1, device_id={"sp": lax.rem(me + k, n)}, device_id_type=LOGICAL)
        return c

    lax.fori_loop(1, n, greet, 0)
    for k in range(1, t_size):
        pl.semaphore_signal(barrier, inc=1, device_id={"tp": lax.rem(tp + k, t_size)}, device_id_type=LOGICAL)
    pl.semaphore_wait(barrier, n - 1 + t_size - 1)

    def w_copy(src, block, way, to):
        return pltpu.make_async_remote_copy(
            src_ref=src, dst_ref=wbuf.at[block], send_sem=w_send.at[way, block],
            recv_sem=w_recv.at[block], device_id={"sp": to}, device_id_type=LOGICAL)

    def halo_copy(side, start, to):
        return pltpu.make_async_remote_copy(
            src_ref=tok.at[pl.ds(start, HALO), :], dst_ref=halo.at[side], send_sem=h_send.at[side],
            recv_sem=h_recv.at[side], device_id={"sp": to}, device_id_type=LOGICAL)

    def st_copy(slot, to):
        return pltpu.make_async_remote_copy(
            src_ref=stept, dst_ref=sbuf.at[me], send_sem=st_send.at[to],
            recv_sem=st_recv.at[slot], device_id={"sp": to}, device_id_type=LOGICAL)

    up_ok, down_ok = h < high - 1, h > 0
    partner = me + 1 - 2 * l

    @pl.when(up_ok)
    def _():
        w_copy(w, me, 0, me + 2).start()

    @pl.when(down_ok)
    def _():
        w_copy(w, me, 1, me - 2).start()

    w_copy(w, me, 2, partner).start()

    @pl.when(me < n - 1)
    def _():
        halo_copy(0, rows - HALO, me + 1).start()

    @pl.when(me > 0)
    def _():
        halo_copy(1, 0, me - 1).start()

    def send_step(k, c):
        st_copy(me, lax.rem(me + k, n)).start()
        return c

    lax.fori_loop(1, n, send_step, 0)

    def norm(v):
        wide = v.astype(f32)
        return (wide * lax.rsqrt(jnp.mean(wide * wide, axis=1, keepdims=True) + EPSILON)
                * gain[...].astype(f32)).astype(bf16)

    chunk = 64

    def norm_rows(i, c):
        at = pl.multiple_of(i * chunk, chunk)
        xn[pl.ds(pl.multiple_of(HALO + at, HALO), chunk), :] = norm(tok[pl.ds(at, chunk), :])
        return c

    lax.fori_loop(0, rows // chunk, norm_rows, 0)

    @pl.when(me > 0)
    def _():
        halo_copy(0, 0, me).wait_recv()
        xn[0:HALO, :] = norm(halo[0])

    @pl.when(me == 0)
    def _():
        xn[0:HALO, :] = jnp.zeros((HALO, width), bf16)

    @pl.when(me < n - 1)
    def _():
        halo_copy(1, 0, me).wait_recv()
        xn[HALO + rows:, :] = norm(halo[1])

    @pl.when(me == n - 1)
    def _():
        xn[HALO + rows:, :] = jnp.zeros((HALO, width), bf16)

    def project(block, piece):
        at = pl.multiple_of(block * depth, 128)
        acc[...] += jnp.dot(xn[:, pl.ds(at, depth)], piece, preferred_element_type=f32)

    for d in range(1, high):
        @pl.when(h - d >= 0)
        def _():
            block = me - 2 * d
            w_copy(w, block, 0, me).wait_recv()

            @pl.when(up_ok)
            def _():
                w_copy(wbuf.at[block], block, 0, me + 2).start()
            w_copy(wbuf.at[block], block, 2, partner).start()

        @pl.when(h + d < high)
        def _():
            block = me + 2 * d
            w_copy(w, block, 1, me).wait_recv()

            @pl.when(down_ok)
            def _():
                w_copy(wbuf.at[block], block, 1, me - 2).start()
            w_copy(wbuf.at[block], block, 2, partner).start()

    wbuf[me] = w[...]
    sbuf[me] = stept[...]
    acc[...] = jnp.zeros_like(acc)

    def wait_cross(d, c):
        w_copy(w, 2 * d + 1 - l, 2, me).wait_recv()
        return c

    def wait_step(k, c):
        st_copy(lax.rem(me + k, n), me).wait_recv()
        return c

    lax.fori_loop(1, n, wait_step, 0)
    per = max(1, 256 // depth)

    if depth % 128 == 0:
        def own_half(i, c):
            block = 2 * lax.rem(h + i, high) + l
            project(block, wbuf[block])
            return c

        def other_half(i, c):
            d = lax.rem(h + i, high)
            wait_cross(d, 0)
            block = 2 * d + 1 - l
            project(block, wbuf[block])
            return c

        lax.fori_loop(0, high, own_half, 0)
        lax.fori_loop(0, high, other_half, 0)
    else:
        lax.fori_loop(0, high, wait_cross, 0)

        def joined(i, c):
            block = wbuf[pl.ds(i * per, per)].reshape(per * depth, wbuf.shape[2])
            at = pl.multiple_of(i * (per * depth), per * depth)
            acc[...] += jnp.dot(xn[:, pl.ds(at, per * depth)], block, preferred_element_type=f32)
            return c

        lax.fori_loop(0, n // per, joined, 0)

    stepw = jnp.concatenate([sbuf[i][:, :depth] for i in range(n)], axis=1)
    raw = lax.dot_general(stepw, xn[HALO:HALO + rows, :], (((1,), (1,)), ((), ())), preferred_element_type=f32)
    step = base[...] * softplus(raw) * psf[...]
    decay = pld[...] - step
    at_s = lax.broadcasted_iota(jnp.int32, (rows, rows), 1)
    at_t = lax.broadcasted_iota(jnp.int32, (rows, rows), 0)
    upper = (at_t <= at_s).astype(f32)
    run = lax.dot_general(decay, upper, (((1,), (0,)), ((), ())), precision=HIGHEST, preferred_element_type=f32)
    before = run - decay
    total = run[:, rows - 1:rows]
    run_c = run.T
    before_c = before.T

    acc[...] = acc[...].astype(bf16).astype(f32)
    third = inner + 2 * state
    mixed_in = (acc[HALO - 1:HALO - 1 + rows, 0:third] * taps[0:1, :].astype(f32)
                + acc[HALO:HALO + rows, 0:third] * taps[1:2, :].astype(f32)
                + acc[HALO + 1:HALO + 1 + rows, 0:third] * taps[2:3, :].astype(f32))
    active = silu(mixed_in)
    inputs = active[:, 0:inner].astype(bf16)
    writers = active[:, inner:inner + state].astype(bf16)
    readers = active[:, inner + state:third].astype(bf16)
    writers_t = writers.astype(f32).T

    heads = inner // HEAD_DIM
    lane_head = lax.broadcasted_iota(jnp.int32, (1, inner), 1) // HEAD_DIM
    picked = [jnp.where(lane_head == i, inputs.astype(f32), 0.0).astype(bf16) for i in range(heads)]

    fade = jnp.exp(total - run) * step
    lead = jnp.exp(before) * step
    s_f = jnp.zeros((state, inner), f32)
    s_b = jnp.zeros((state, inner), f32)
    tot_row = jnp.zeros((1, inner), f32)
    for i in range(heads):
        s_f += jnp.dot((writers_t * fade[i:i + 1, :]).astype(bf16), picked[i], preferred_element_type=f32)
        s_b += jnp.dot((writers_t * lead[i:i + 1, :]).astype(bf16), picked[i], preferred_element_type=f32)
        tot_row = jnp.where(lane_head == i, total[i:i + 1, :], tot_row)
    s_out[0] = s_f.astype(bf16)
    s_out[1] = s_b.astype(bf16)
    tot_out[...] = jnp.broadcast_to(tot_row, tot_out.shape)

    def s_copy(which, slot, to):
        return pltpu.make_async_remote_copy(
            src_ref=s_out.at[which], dst_ref=s_in.at[me], send_sem=s_send.at[to],
            recv_sem=s_recv.at[slot], device_id={"sp": to}, device_id_type=LOGICAL)

    def tot_copy(slot, to):
        return pltpu.make_async_remote_copy(
            src_ref=tot_out, dst_ref=tot_in.at[me], send_sem=t_send.at[to],
            recv_sem=t_recv.at[slot], device_id={"sp": to}, device_id_type=LOGICAL)

    def send_up(to, c):
        s_copy(0, me, to).start()
        tot_copy(me, to).start()
        return c

    def send_down(k, c):
        s_copy(1, me, me - 1 - k).start()
        tot_copy(me, me - 1 - k).start()
        return c

    lax.fori_loop(me + 1, n, send_up, 0)
    lax.fori_loop(0, me, send_down, 0)

    pool_at = third + inner
    half = lax.shift_left(jnp.int32(1), tp)
    ext = rows + 2 * HALO
    off = lax.broadcasted_iota(jnp.int32, (rows, ext), 1) - HALO - lax.broadcasted_iota(jnp.int32, (rows, ext), 0)
    band = jnp.where((off >= -half) & (off < half), 1.0, 0.0).astype(bf16)
    window = jnp.dot(band, acc[:, pool_at:pool_at + pool].astype(bf16), preferred_element_type=f32)
    position = me * rows + lax.broadcasted_iota(jnp.int32, (rows, 1), 0)
    count = (jnp.minimum(position + half, rows * n) - jnp.maximum(position - half, 0)).astype(f32)
    pooled = (window / count - acc[HALO:HALO + rows, pool_at:pool_at + pool]).astype(bf16)
    pool_mixed = (jnp.dot(pooled, maps[...], preferred_element_type=f32) * pscale[...].astype(f32)).astype(bf16)
    tile = rows // t_size
    for j in range(t_size):
        xs[j, :, inner:inner + pool] = pool_mixed[j * tile:(j + 1) * tile]

    scores = lax.dot_general(readers, writers, (((1,), (1,)), ((), ())), preferred_element_type=f32)
    scores = jnp.where(at_s == at_t, 2.0 * scores, scores)
    scanned = jnp.zeros((rows, inner), f32)
    for i in range(heads):
        spread = jnp.where(at_s <= at_t, run_c[:, i:i + 1] - run[i:i + 1, :],
                           before[i:i + 1, :] - before_c[:, i:i + 1])
        weights = (scores * (jnp.exp(spread) * step[i:i + 1, :])).astype(bf16)
        scanned += jnp.dot(weights, picked[i], preferred_element_type=f32)

    run_x = jnp.zeros((rows, inner), f32)
    left_x = jnp.zeros((rows, inner), f32)
    for i in range(heads):
        run_x = jnp.where(lane_head == i, run_c[:, i:i + 1], run_x)
        left_x = jnp.where(lane_head == i, total[i:i + 1, :] - before_c[:, i:i + 1], left_x)

    ent[...] = jnp.zeros_like(ent)
    lea[...] = jnp.zeros_like(lea)

    def take_wait(i):
        pltpu.make_async_remote_copy(
            src_ref=s_out.at[0], dst_ref=s_in.at[i], send_sem=s_send.at[i],
            recv_sem=s_recv.at[i], device_id={"sp": i}, device_id_type=LOGICAL).wait_recv()
        pltpu.make_async_remote_copy(
            src_ref=tot_out, dst_ref=tot_in.at[i], send_sem=t_send.at[i],
            recv_sem=t_recv.at[i], device_id={"sp": i}, device_id_type=LOGICAL).wait_recv()

    def enter(i, c):
        take_wait(i)
        ent[...] = ent[...] * jnp.exp(tot_in[i][0:1, :]) + s_in[i].astype(f32)
        return c

    def leave(k, c):
        i = n - 1 - k
        take_wait(i)
        lea[...] = lea[...] * jnp.exp(tot_in[i][0:1, :]) + s_in[i].astype(f32)
        return c

    lax.fori_loop(0, me, enter, 0)
    lax.fori_loop(0, n - 1 - me, leave, 0)
    scanned += jnp.dot(readers, ent[...].astype(bf16), preferred_element_type=f32) * jnp.exp(run_x)
    scanned += jnp.dot(readers, lea[...].astype(bf16), preferred_element_type=f32) * jnp.exp(left_x)

    gated = scanned * silu(acc[HALO:HALO + rows, third:third + inner])
    square = lax.dot_general(jnp.ones((8, inner), f32), gated * gated, (((1,), (1,)), ((), ())),
                             precision=HIGHEST, preferred_element_type=f32)
    scaled = (gated * ngain[...].astype(f32)).astype(bf16)
    for j in range(t_size):
        xs[j, :, 0:inner] = scaled[j * tile:(j + 1) * tile]
        qs[j] = square[:, j * tile:(j + 1) * tile]

    def x_copy(slot, to):
        return pltpu.make_async_remote_copy(
            src_ref=xs.at[to], dst_ref=xr.at[slot], send_sem=x_send.at[to],
            recv_sem=x_recv.at[slot], device_id={"tp": to}, device_id_type=LOGICAL)

    def q_copy(slot, to):
        return pltpu.make_async_remote_copy(
            src_ref=qs.at[to], dst_ref=qr.at[slot], send_sem=q_send.at[to],
            recv_sem=q_recv.at[slot], device_id={"tp": to}, device_id_type=LOGICAL)

    for k in range(1, t_size):
        to = lax.rem(tp + k, t_size)
        q_copy(tp, to).start()
        x_copy(tp, to).start()
    xr[tp] = xs[tp]
    qr[tp] = qs[tp]
    for k in range(1, t_size):
        frm = lax.rem(tp + k, t_size)
        q_copy(frm, frm).wait_recv()
        x_copy(frm, frm).wait_recv()
    sums = qr[0]
    for j in range(1, t_size):
        sums = sums + qr[j]
    factor = lax.rsqrt(sums.T[:, 0:1] / SSD_INNER + EPSILON)
    both = inner + pool
    for j in range(t_size):
        out[:, j * both:j * both + inner] = (xr[j, :, 0:inner].astype(f32) * factor).astype(bf16)
        out[:, j * both + inner:(j + 1) * both] = xr[j, :, inner:both]

    @pl.when(up_ok)
    def _():
        w_copy(w, me, 0, me + 2).wait_send()

    @pl.when(down_ok)
    def _():
        w_copy(w, me, 1, me - 2).wait_send()

    w_copy(w, me, 2, partner).wait_send()
    for d in range(1, high):
        @pl.when(h - d >= 0)
        def _():
            block = me - 2 * d

            @pl.when(up_ok)
            def _():
                w_copy(w, block, 0, me + 2).wait_send()
            w_copy(w, block, 2, partner).wait_send()

        @pl.when(h + d < high)
        def _():
            block = me + 2 * d

            @pl.when(down_ok)
            def _():
                w_copy(w, block, 1, me - 2).wait_send()
            w_copy(w, block, 2, partner).wait_send()

    @pl.when(me < n - 1)
    def _():
        halo_copy(0, rows - HALO, me + 1).wait_send()

    @pl.when(me > 0)
    def _():
        halo_copy(1, 0, me - 1).wait_send()

    def sent(k, c):
        to = lax.rem(me + k, n)
        st_copy(me, to).wait_send()
        s_copy(0, me, to).wait_send()
        tot_copy(me, to).wait_send()
        return c

    lax.fori_loop(1, n, sent, 0)
    for k in range(1, t_size):
        to = lax.rem(tp + k, t_size)
        q_copy(tp, to).wait_send()
        x_copy(tp, to).wait_send()


def shards(
    tokens, input_norm_gain, gate_matrix, input_matrix, write_matrix, read_matrix, step_matrix,
    pooling_input_matrix, input_conv_taps, write_conv_taps, read_conv_taps, head_step_base,
    position_step_factor, position_log_decay, gated_norm_gain, group_linear_maps,
    pooling_channel_scale, state_output_matrix, pooling_output_matrix,
):
    n, t_size = lax.axis_size("sp"), lax.axis_size("tp")
    rows, width = tokens.shape
    inner, state, pool = input_matrix.shape[1], write_matrix.shape[1], pooling_input_matrix.shape[1]
    depth = input_matrix.shape[0]
    heads = head_step_base.shape[0]
    out_w = jnp.concatenate((state_output_matrix, pooling_output_matrix), axis=0)
    out_w = lax.all_gather(out_w, "sp", axis=1, tiled=True)
    out_w = lax.all_gather(out_w, "tp", axis=0, tiled=True)

    w = jnp.concatenate((input_matrix, write_matrix, read_matrix, gate_matrix, pooling_input_matrix), axis=1)
    pad = 16 - heads
    own = lax.dynamic_slice_in_dim(step_matrix, lax.axis_index("tp") * heads, heads, 1)
    stept = jnp.pad(own.T, ((0, pad), (0, max(0, 128 - depth))))
    taps = jnp.concatenate((input_conv_taps, write_conv_taps, read_conv_taps), axis=1)
    base = jnp.pad(head_step_base, (0, pad))[:, None]
    pld = jnp.pad(position_log_decay.T, ((0, pad), (0, 0)))
    ext, cols, both = rows + 2 * HALO, w.shape[1], inner + pool
    tile = rows // t_size
    vmem = pl.BlockSpec(memory_space=pltpu.VMEM)
    dma = pltpu.SemaphoreType.DMA
    x = pl.pallas_call(
        functools.partial(mixer_kernel, n, t_size, (rows, inner, state, pool)),
        out_shape=jax.ShapeDtypeStruct((tile, t_size * both), bf16),
        in_specs=[vmem] * 11,
        out_specs=vmem,
        scratch_shapes=[
            pltpu.VMEM((2, HALO, width), bf16),
            pltpu.VMEM((ext, width), bf16),
            pltpu.VMEM((n, depth, cols), bf16),
            pltpu.VMEM((n, 16, stept.shape[1]), bf16),
            pltpu.VMEM((ext, cols), f32),
            pltpu.VMEM((2, state, inner), bf16),
            pltpu.VMEM((n, state, inner), bf16),
            pltpu.VMEM((8, inner), f32),
            pltpu.VMEM((n, 8, inner), f32),
            pltpu.VMEM((state, inner), f32),
            pltpu.VMEM((state, inner), f32),
            pltpu.VMEM((t_size, tile, both), bf16),
            pltpu.VMEM((t_size, tile, both), bf16),
            pltpu.VMEM((t_size, 8, tile), f32),
            pltpu.VMEM((t_size, 8, tile), f32),
            dma((3, n)), dma((n,)), dma((n,)), dma((n,)), dma((2,)), dma((2,)),
            dma((n,)), dma((n,)), dma((n,)), dma((n,)),
            dma((t_size,)), dma((t_size,)), dma((t_size,)), dma((t_size,)),
        ],
        compiler_params=pltpu.CompilerParams(
            collective_id=0, has_side_effects=True, vmem_limit_bytes=56 * 1024 * 1024),
        cost_estimate=pl.CostEstimate(flops=100_000_000_000, bytes_accessed=16_000_000, transcendentals=0),
    )(tokens, input_norm_gain[None, :], w, stept, taps, base, position_step_factor[None, :], pld,
      gated_norm_gain[None, :], group_linear_maps[0], pooling_channel_scale[None, :])
    return jnp.dot(x, out_w, preferred_element_type=f32).astype(bf16)


def solution(mesh):
    placed = (
        P("sp", None), P(), P("sp", "tp"), P("sp", "tp"), P("sp", "tp"), P("sp", "tp"), P("sp", None),
        P("sp", "tp"), P(None, "tp"), P(None, "tp"), P(None, "tp"), P("tp"), P("sp"), P("sp", "tp"),
        P("tp"), P("tp", None, None), P("tp"), P("tp", "sp"), P("tp", "sp"),
    )
    return jax.shard_map(
        shards, mesh=mesh, in_specs=placed, out_specs=P(("sp", "tp"), None), check_vma=False)
```

```python
import functools

import jax
import jax.numpy as jnp
from jax import lax
from jax.experimental import pallas as pl
from jax.experimental.pallas import tpu as pltpu
from jax.sharding import PartitionSpec as P

HEAD_DIM = 64
SSD_INNER = 1024
EPSILON = 1e-06
HALO = 16
LOGICAL = pl.DeviceIdType.MESH
f32 = jnp.float32
bf16 = jnp.bfloat16
HIGHEST = lax.Precision.HIGHEST


def softplus(v):
    return jnp.maximum(v, 0.0) + jnp.log1p(jnp.exp(-jnp.abs(v)))


def silu(v):
    return v / (1.0 + jnp.exp(-v))


def mixer_kernel(
    n, t_size, dims,
    tok, gain, w, stept, taps, base, psf, pld, ngain, maps, pscale,
    out,
    halo, xn, wbuf, sbuf, acc, s_out, s_in, tot_out, tot_in, ent, lea, xs, xr, qs, qr,
    w_send, w_recv, st_send, st_recv, h_send, h_recv, s_send, s_recv, t_send, t_recv,
    x_send, x_recv, q_send, q_recv,
):
    rows, inner, state, pool = dims
    me = lax.axis_index("sp")
    tp = lax.axis_index("tp")
    high = n // 2
    h, l = me // 2, me % 2
    depth = w.shape[0]
    width = tok.shape[1]

    barrier = pltpu.get_barrier_semaphore()

    def greet(k, c):
        pl.semaphore_signal(barrier, inc=1, device_id={"sp": lax.rem(me + k, n)}, device_id_type=LOGICAL)
        return c

    lax.fori_loop(1, n, greet, 0)
    for k in range(1, t_size):
        pl.semaphore_signal(barrier, inc=1, device_id={"tp": lax.rem(tp + k, t_size)}, device_id_type=LOGICAL)
    pl.semaphore_wait(barrier, n - 1 + t_size - 1)

    def w_copy(src, block, way, to):
        return pltpu.make_async_remote_copy(
            src_ref=src, dst_ref=wbuf.at[block], send_sem=w_send.at[way, block],
            recv_sem=w_recv.at[block], device_id={"sp": to}, device_id_type=LOGICAL)

    def halo_copy(side, start, to):
        return pltpu.make_async_remote_copy(
            src_ref=tok.at[pl.ds(start, HALO), :], dst_ref=halo.at[side], send_sem=h_send.at[side],
            recv_sem=h_recv.at[side], device_id={"sp": to}, device_id_type=LOGICAL)

    def st_copy(slot, to):
        return pltpu.make_async_remote_copy(
            src_ref=stept, dst_ref=sbuf.at[me], send_sem=st_send.at[to],
            recv_sem=st_recv.at[slot], device_id={"sp": to}, device_id_type=LOGICAL)

    up_ok, down_ok = h < high - 1, h > 0
    partner = me + 1 - 2 * l

    @pl.when(up_ok)
    def _():
        w_copy(w, me, 0, me + 2).start()

    @pl.when(down_ok)
    def _():
        w_copy(w, me, 1, me - 2).start()

    w_copy(w, me, 2, partner).start()

    @pl.when(me < n - 1)
    def _():
        halo_copy(0, rows - HALO, me + 1).start()

    @pl.when(me > 0)
    def _():
        halo_copy(1, 0, me - 1).start()

    def send_step(k, c):
        st_copy(me, lax.rem(me + k, n)).start()
        return c

    lax.fori_loop(1, n, send_step, 0)

    def norm(v):
        wide = v.astype(f32)
        return (wide * lax.rsqrt(jnp.mean(wide * wide, axis=1, keepdims=True) + EPSILON)
                * gain[...].astype(f32)).astype(bf16)

    chunk = 64

    def norm_rows(i, c):
        at = pl.multiple_of(i * chunk, chunk)
        xn[pl.ds(pl.multiple_of(HALO + at, HALO), chunk), :] = norm(tok[pl.ds(at, chunk), :])
        return c

    lax.fori_loop(0, rows // chunk, norm_rows, 0)

    @pl.when(me > 0)
    def _():
        halo_copy(0, 0, me).wait_recv()
        xn[0:HALO, :] = norm(halo[0])

    @pl.when(me == 0)
    def _():
        xn[0:HALO, :] = jnp.zeros((HALO, width), bf16)

    @pl.when(me < n - 1)
    def _():
        halo_copy(1, 0, me).wait_recv()
        xn[HALO + rows:, :] = norm(halo[1])

    @pl.when(me == n - 1)
    def _():
        xn[HALO + rows:, :] = jnp.zeros((HALO, width), bf16)

    def project(block, piece):
        at = pl.multiple_of(block * depth, 128)
        acc[...] += jnp.dot(xn[:, pl.ds(at, depth)], piece, preferred_element_type=f32)

    for d in range(1, high):
        @pl.when(h - d >= 0)
        def _():
            block = me - 2 * d
            w_copy(w, block, 0, me).wait_recv()

            @pl.when(up_ok)
            def _():
                w_copy(wbuf.at[block], block, 0, me + 2).start()
            w_copy(wbuf.at[block], block, 2, partner).start()

        @pl.when(h + d < high)
        def _():
            block = me + 2 * d
            w_copy(w, block, 1, me).wait_recv()

            @pl.when(down_ok)
            def _():
                w_copy(wbuf.at[block], block, 1, me - 2).start()
            w_copy(wbuf.at[block], block, 2, partner).start()

    wbuf[me] = w[...]
    sbuf[me] = stept[...]
    acc[...] = jnp.zeros_like(acc)

    def wait_cross(d, c):
        w_copy(w, 2 * d + 1 - l, 2, me).wait_recv()
        return c

    def wait_step(k, c):
        st_copy(lax.rem(me + k, n), me).wait_recv()
        return c

    lax.fori_loop(1, n, wait_step, 0)
    per = max(1, 256 // depth)

    if depth % 128 == 0:
        def own_half(i, c):
            block = 2 * lax.rem(h + i, high) + l
            project(block, wbuf[block])
            return c

        def other_half(i, c):
            d = lax.rem(h + i, high)
            wait_cross(d, 0)
            block = 2 * d + 1 - l
            project(block, wbuf[block])
            return c

        lax.fori_loop(0, high, own_half, 0)
        lax.fori_loop(0, high, other_half, 0)
    else:
        lax.fori_loop(0, high, wait_cross, 0)

        def joined(i, c):
            block = wbuf[pl.ds(i * per, per)].reshape(per * depth, wbuf.shape[2])
            at = pl.multiple_of(i * (per * depth), per * depth)
            acc[...] += jnp.dot(xn[:, pl.ds(at, per * depth)], block, preferred_element_type=f32)
            return c

        lax.fori_loop(0, n // per, joined, 0)

    stepw = jnp.concatenate([sbuf[i][:, :depth] for i in range(n)], axis=1)
    raw = lax.dot_general(stepw, xn[HALO:HALO + rows, :], (((1,), (1,)), ((), ())), preferred_element_type=f32)
    step = base[...] * softplus(raw) * psf[...]
    decay = pld[...] - step
    at_s = lax.broadcasted_iota(jnp.int32, (rows, rows), 1)
    at_t = lax.broadcasted_iota(jnp.int32, (rows, rows), 0)
    upper = (at_t <= at_s).astype(f32)
    run = lax.dot_general(decay, upper, (((1,), (0,)), ((), ())), precision=HIGHEST, preferred_element_type=f32)
    before = run - decay
    total = run[:, rows - 1:rows]
    run_c = run.T
    before_c = before.T

    acc[...] = acc[...].astype(bf16).astype(f32)
    third = inner + 2 * state
    mixed_in = (acc[HALO - 1:HALO - 1 + rows, 0:third] * taps[0:1, :].astype(f32)
                + acc[HALO:HALO + rows, 0:third] * taps[1:2, :].astype(f32)
                + acc[HALO + 1:HALO + 1 + rows, 0:third] * taps[2:3, :].astype(f32))
    active = silu(mixed_in)
    inputs = active[:, 0:inner].astype(bf16)
    writers = active[:, inner:inner + state].astype(bf16)
    readers = active[:, inner + state:third].astype(bf16)
    writers_t = writers.astype(f32).T

    heads = inner // HEAD_DIM
    lane_head = lax.broadcasted_iota(jnp.int32, (1, inner), 1) // HEAD_DIM
    picked = [jnp.where(lane_head == i, inputs.astype(f32), 0.0).astype(bf16) for i in range(heads)]

    fade = jnp.exp(total - run) * step
    lead = jnp.exp(before) * step
    s_f = jnp.zeros((state, inner), f32)
    s_b = jnp.zeros((state, inner), f32)
    tot_row = jnp.zeros((1, inner), f32)
    for i in range(heads):
        s_f += jnp.dot((writers_t * fade[i:i + 1, :]).astype(bf16), picked[i], preferred_element_type=f32)
        s_b += jnp.dot((writers_t * lead[i:i + 1, :]).astype(bf16), picked[i], preferred_element_type=f32)
        tot_row = jnp.where(lane_head == i, total[i:i + 1, :], tot_row)
    s_out[0] = s_f.astype(bf16)
    s_out[1] = s_b.astype(bf16)
    tot_out[...] = jnp.broadcast_to(tot_row, tot_out.shape)

    def s_copy(which, slot, to):
        return pltpu.make_async_remote_copy(
            src_ref=s_out.at[which], dst_ref=s_in.at[me], send_sem=s_send.at[to],
            recv_sem=s_recv.at[slot], device_id={"sp": to}, device_id_type=LOGICAL)

    def tot_copy(slot, to):
        return pltpu.make_async_remote_copy(
            src_ref=tot_out, dst_ref=tot_in.at[me], send_sem=t_send.at[to],
            recv_sem=t_recv.at[slot], device_id={"sp": to}, device_id_type=LOGICAL)

    def send_up(to, c):
        s_copy(0, me, to).start()
        tot_copy(me, to).start()
        return c

    def send_down(k, c):
        s_copy(1, me, me - 1 - k).start()
        tot_copy(me, me - 1 - k).start()
        return c

    lax.fori_loop(me + 1, n, send_up, 0)
    lax.fori_loop(0, me, send_down, 0)

    pool_at = third + inner
    half = lax.shift_left(jnp.int32(1), tp)
    ext = rows + 2 * HALO
    off = lax.broadcasted_iota(jnp.int32, (rows, ext), 1) - HALO - lax.broadcasted_iota(jnp.int32, (rows, ext), 0)
    band = jnp.where((off >= -half) & (off < half), 1.0, 0.0).astype(bf16)
    window = jnp.dot(band, acc[:, pool_at:pool_at + pool].astype(bf16), preferred_element_type=f32)
    position = me * rows + lax.broadcasted_iota(jnp.int32, (rows, 1), 0)
    count = (jnp.minimum(position + half, rows * n) - jnp.maximum(position - half, 0)).astype(f32)
    pooled = (window / count - acc[HALO:HALO + rows, pool_at:pool_at + pool]).astype(bf16)
    pool_mixed = (jnp.dot(pooled, maps[...], preferred_element_type=f32) * pscale[...].astype(f32)).astype(bf16)
    tile = rows // t_size
    for j in range(t_size):
        xs[j, :, inner:inner + pool] = pool_mixed[j * tile:(j + 1) * tile]

    scores = lax.dot_general(readers, writers, (((1,), (1,)), ((), ())), preferred_element_type=f32)
    scores = jnp.where(at_s == at_t, 2.0 * scores, scores)
    scanned = jnp.zeros((rows, inner), f32)
    for i in range(heads):
        spread = jnp.where(at_s <= at_t, run_c[:, i:i + 1] - run[i:i + 1, :],
                           before[i:i + 1, :] - before_c[:, i:i + 1])
        weights = (scores * (jnp.exp(spread) * step[i:i + 1, :])).astype(bf16)
        scanned += jnp.dot(weights, picked[i], preferred_element_type=f32)

    run_x = jnp.zeros((rows, inner), f32)
    left_x = jnp.zeros((rows, inner), f32)
    for i in range(heads):
        run_x = jnp.where(lane_head == i, run_c[:, i:i + 1], run_x)
        left_x = jnp.where(lane_head == i, total[i:i + 1, :] - before_c[:, i:i + 1], left_x)

    ent[...] = jnp.zeros_like(ent)
    lea[...] = jnp.zeros_like(lea)

    def take_wait(i):
        pltpu.make_async_remote_copy(
            src_ref=s_out.at[0], dst_ref=s_in.at[i], send_sem=s_send.at[i],
            recv_sem=s_recv.at[i], device_id={"sp": i}, device_id_type=LOGICAL).wait_recv()
        pltpu.make_async_remote_copy(
            src_ref=tot_out, dst_ref=tot_in.at[i], send_sem=t_send.at[i],
            recv_sem=t_recv.at[i], device_id={"sp": i}, device_id_type=LOGICAL).wait_recv()

    def enter(i, c):
        take_wait(i)
        ent[...] = ent[...] * jnp.exp(tot_in[i][0:1, :]) + s_in[i].astype(f32)
        return c

    def leave(k, c):
        i = n - 1 - k
        take_wait(i)
        lea[...] = lea[...] * jnp.exp(tot_in[i][0:1, :]) + s_in[i].astype(f32)
        return c

    lax.fori_loop(0, me, enter, 0)
    lax.fori_loop(0, n - 1 - me, leave, 0)
    scanned += jnp.dot(readers, ent[...].astype(bf16), preferred_element_type=f32) * jnp.exp(run_x)
    scanned += jnp.dot(readers, lea[...].astype(bf16), preferred_element_type=f32) * jnp.exp(left_x)

    gated = scanned * silu(acc[HALO:HALO + rows, third:third + inner])
    square = lax.dot_general(jnp.ones((8, inner), f32), gated * gated, (((1,), (1,)), ((), ())),
                             precision=HIGHEST, preferred_element_type=f32)
    scaled = (gated * ngain[...].astype(f32)).astype(bf16)
    for j in range(t_size):
        xs[j, :, 0:inner] = scaled[j * tile:(j + 1) * tile]
        qs[j] = square[:, j * tile:(j + 1) * tile]

    def x_copy(slot, to):
        return pltpu.make_async_remote_copy(
            src_ref=xs.at[to], dst_ref=xr.at[slot], send_sem=x_send.at[to],
            recv_sem=x_recv.at[slot], device_id={"tp": to}, device_id_type=LOGICAL)

    def q_copy(slot, to):
        return pltpu.make_async_remote_copy(
            src_ref=qs.at[to], dst_ref=qr.at[slot], send_sem=q_send.at[to],
            recv_sem=q_recv.at[slot], device_id={"tp": to}, device_id_type=LOGICAL)

    for k in range(1, t_size):
        to = lax.rem(tp + k, t_size)
        q_copy(tp, to).start()
        x_copy(tp, to).start()
    xr[tp] = xs[tp]
    qr[tp] = qs[tp]
    for k in range(1, t_size):
        frm = lax.rem(tp + k, t_size)
        q_copy(frm, frm).wait_recv()
        x_copy(frm, frm).wait_recv()
    sums = qr[0]
    for j in range(1, t_size):
        sums = sums + qr[j]
    factor = lax.rsqrt(sums.T[:, 0:1] / SSD_INNER + EPSILON)
    both = inner + pool
    for j in range(t_size):
        out[:, j * both:j * both + inner] = (xr[j, :, 0:inner].astype(f32) * factor).astype(bf16)
        out[:, j * both + inner:(j + 1) * both] = xr[j, :, inner:both]

    @pl.when(up_ok)
    def _():
        w_copy(w, me, 0, me + 2).wait_send()

    @pl.when(down_ok)
    def _():
        w_copy(w, me, 1, me - 2).wait_send()

    w_copy(w, me, 2, partner).wait_send()
    for d in range(1, high):
        @pl.when(h - d >= 0)
        def _():
            block = me - 2 * d

            @pl.when(up_ok)
            def _():
                w_copy(w, block, 0, me + 2).wait_send()
            w_copy(w, block, 2, partner).wait_send()

        @pl.when(h + d < high)
        def _():
            block = me + 2 * d

            @pl.when(down_ok)
            def _():
                w_copy(w, block, 1, me - 2).wait_send()
            w_copy(w, block, 2, partner).wait_send()

    @pl.when(me < n - 1)
    def _():
        halo_copy(0, rows - HALO, me + 1).wait_send()

    @pl.when(me > 0)
    def _():
        halo_copy(1, 0, me - 1).wait_send()

    def sent(k, c):
        to = lax.rem(me + k, n)
        st_copy(me, to).wait_send()
        s_copy(0, me, to).wait_send()
        tot_copy(me, to).wait_send()
        return c

    lax.fori_loop(1, n, sent, 0)
    for k in range(1, t_size):
        to = lax.rem(tp + k, t_size)
        q_copy(tp, to).wait_send()
        x_copy(tp, to).wait_send()


def shards(
    tokens, input_norm_gain, gate_matrix, input_matrix, write_matrix, read_matrix, step_matrix,
    pooling_input_matrix, input_conv_taps, write_conv_taps, read_conv_taps, head_step_base,
    position_step_factor, position_log_decay, gated_norm_gain, group_linear_maps,
    pooling_channel_scale, state_output_matrix, pooling_output_matrix,
):
    n, t_size = lax.axis_size("sp"), lax.axis_size("tp")
    rows, width = tokens.shape
    inner, state, pool = input_matrix.shape[1], write_matrix.shape[1], pooling_input_matrix.shape[1]
    depth = input_matrix.shape[0]
    heads = head_step_base.shape[0]
    out_w = jnp.concatenate((state_output_matrix, pooling_output_matrix), axis=0)
    out_w = lax.all_gather(out_w, ("sp", "tp"), axis=0, tiled=True)
    out_w = out_w.reshape(n, -1, out_w.shape[1])

    w = jnp.concatenate((input_matrix, write_matrix, read_matrix, gate_matrix, pooling_input_matrix), axis=1)
    pad = 16 - heads
    own = lax.dynamic_slice_in_dim(step_matrix, lax.axis_index("tp") * heads, heads, 1)
    stept = jnp.pad(own.T, ((0, pad), (0, max(0, 128 - depth))))
    taps = jnp.concatenate((input_conv_taps, write_conv_taps, read_conv_taps), axis=1)
    base = jnp.pad(head_step_base, (0, pad))[:, None]
    pld = jnp.pad(position_log_decay.T, ((0, pad), (0, 0)))
    ext, cols, both = rows + 2 * HALO, w.shape[1], inner + pool
    tile = rows // t_size
    vmem = pl.BlockSpec(memory_space=pltpu.VMEM)
    dma = pltpu.SemaphoreType.DMA
    x = pl.pallas_call(
        functools.partial(mixer_kernel, n, t_size, (rows, inner, state, pool)),
        out_shape=jax.ShapeDtypeStruct((tile, t_size * both), bf16),
        in_specs=[vmem] * 11,
        out_specs=vmem,
        scratch_shapes=[
            pltpu.VMEM((2, HALO, width), bf16),
            pltpu.VMEM((ext, width), bf16),
            pltpu.VMEM((n, depth, cols), bf16),
            pltpu.VMEM((n, 16, stept.shape[1]), bf16),
            pltpu.VMEM((ext, cols), f32),
            pltpu.VMEM((2, state, inner), bf16),
            pltpu.VMEM((n, state, inner), bf16),
            pltpu.VMEM((8, inner), f32),
            pltpu.VMEM((n, 8, inner), f32),
            pltpu.VMEM((state, inner), f32),
            pltpu.VMEM((state, inner), f32),
            pltpu.VMEM((t_size, tile, both), bf16),
            pltpu.VMEM((t_size, tile, both), bf16),
            pltpu.VMEM((t_size, 8, tile), f32),
            pltpu.VMEM((t_size, 8, tile), f32),
            dma((3, n)), dma((n,)), dma((n,)), dma((n,)), dma((2,)), dma((2,)),
            dma((n,)), dma((n,)), dma((n,)), dma((n,)),
            dma((t_size,)), dma((t_size,)), dma((t_size,)), dma((t_size,)),
        ],
        compiler_params=pltpu.CompilerParams(
            collective_id=0, has_side_effects=True, vmem_limit_bytes=56 * 1024 * 1024),
        cost_estimate=pl.CostEstimate(flops=100_000_000_000, bytes_accessed=16_000_000, transcendentals=0),
    )(tokens, input_norm_gain[None, :], w, stept, taps, base, position_step_factor[None, :], pld,
      gated_norm_gain[None, :], group_linear_maps[0], pooling_channel_scale[None, :])
    mixed = jnp.einsum("tk,skc->tsc", x, out_w, preferred_element_type=f32)
    return mixed.astype(bf16).reshape(tile, -1)


def solution(mesh):
    placed = (
        P("sp", None), P(), P("sp", "tp"), P("sp", "tp"), P("sp", "tp"), P("sp", "tp"), P("sp", None),
        P("sp", "tp"), P(None, "tp"), P(None, "tp"), P(None, "tp"), P("tp"), P("sp"), P("sp", "tp"),
        P("tp"), P("tp", None, None), P("tp"), P("tp", "sp"), P("tp", "sp"),
    )
    return jax.shard_map(
        shards, mesh=mesh, in_specs=placed, out_specs=P(("sp", "tp"), None), check_vma=False)
```
